256 devices in a mesh: rep: 2 (over z_hi), fs: 16 (over z_lo, x), tp: 8 (over y, core).
Axes of the slice: x: 4, y: 4, z: 8 (z_hi: 2, z_lo: 4; z = z_hi * 4 + z_lo), core: 2. Of those that a mesh axis runs over, the one named last changes fastest.
Arguments:
- tokens: bfloat16 [32768, 2048], P(('rep', 'fs', 'tp')), may hold values from -6 to 6
- norm1_gain: float32 [2048], replicated, may hold values from 0.1 to 1.9
- in_weight: bfloat16 [2048, 1024], P('fs', 'tp'), may hold values from -0.125 to 0.125
- group_weight: bfloat16 [8, 128, 128], P('tp'), may hold values from -0.5 to 0.5
- pool_scale: float32 [1024], P('tp'), may hold values from 0.1 to 1.9
- out_weight: bfloat16 [1024, 2048], P('tp', 'fs'), may hold values from -0.1875 to 0.1875
- norm2_gain: float32 [2048], replicated, may hold values from 0.1 to 1.9
- up_weight: bfloat16 [2048, 8192], P('fs', 'tp'), may hold values from -0.125 to 0.125
- down_weight: bfloat16 [8192, 2048], P('tp', 'fs'), may hold values from -0.0625 to 0.0625
Outputs:
- layer_out: bfloat16 [32768, 2048], P(('rep', 'fs', 'tp'))
The draws below stay inside these ranges and needn't reach their ends.
All inputs are finite; a program needn't handle non-finite values.
Results may differ from the reference program's by a relative error of at most 0.02.
Values may be sent and summed in bfloat16 or wider, within the bound.
No kernel may reach another device: no remote copies, remote signals or barrier semaphores. Data moves between devices by JAX's collectives and lax.ppermute only.
A program may use at most 128 MiB of HBM per device.

```python
import jax
import jax.numpy as jnp
from jax import lax

D = 2048
GROUPS = 8
GROUP_DIM = 128
FF = 8192
POOL = 1024
SEQ = 1024
TOKENS = 32768
N_TP = 8


def block_levels(own_key, dims, shards, smallest, largest):
    def one(dim, blocks):
        steps = jax.random.uniform(jax.random.fold_in(jax.random.fold_in(own_key, 6), dim), (blocks,), jnp.float32, smallest / len(shards), largest / len(shards))
        return jnp.repeat(jnp.exp(steps), dims[dim] // blocks).reshape((-1,) + (1,) * (len(dims) - dim - 1))

    loudness = one(*shards[0])
    for cut in shards[1:]:
        loudness = loudness * one(*cut)
    return loudness


def normal_values(rng, shape, scale, most, cuts=(), kind=jnp.bfloat16):
    values = scale * jax.random.normal(rng, shape, jnp.float32)
    if cuts:
        values = values * block_levels(rng, shape, cuts, -0.22, 0.18)
    return jnp.clip(values, -most, most).astype(kind)


def setup_inputs(seed: int = 0) -> dict:
    streams_of = jax.random.split(jax.random.key(seed), 10)
    return {
        "tokens": normal_values(streams_of[0], (TOKENS, D), 1.0, 6.0, ((0, 256),)),
        "norm1_gain": jnp.clip(1.0 + 0.18 * jax.random.normal(streams_of[1], (D,), jnp.float32), 0.1, 1.9),
        "in_weight": normal_values(streams_of[2], (D, POOL), D ** -0.5, 0.125, ((0, 16), (1, 8))),
        "group_weight": normal_values(streams_of[3], (GROUPS, GROUP_DIM, GROUP_DIM), GROUP_DIM ** -0.5, 0.5, ((0, 8),)),
        "pool_scale": jnp.clip(1.0 + 0.18 * jax.random.normal(streams_of[4], (POOL,), jnp.float32), 0.1, 1.9),
        "out_weight": normal_values(streams_of[5], (POOL, D), POOL ** -0.5, 0.1875, ((0, 8), (1, 16))),
        "norm2_gain": jnp.clip(1.0 + 0.18 * jax.random.normal(streams_of[6], (D,), jnp.float32), 0.1, 1.9),
        "up_weight": normal_values(streams_of[7], (D, FF), D ** -0.5, 0.125, ((0, 16), (1, 8))),
        "down_weight": normal_values(streams_of[8], (FF, D), FF ** -0.5, 0.0625, ((0, 8), (1, 16))),
    }


epsilon = 1e-06

def rms_norm(values, gain):
    scale = lax.rsqrt(lax.optimization_barrier(jnp.mean(values * values, axis=-1, keepdims=True)) + epsilon)
    return values * scale * gain

def one_sequence(rows, norm1_gain, in_weight, group_weight, pool_scale, out_weight, norm2_gain, up_weight, down_weight):
    stream = rows.astype(jnp.float32)
    normed = rms_norm(stream, norm1_gain).astype(jnp.bfloat16)
    projected = jnp.dot(normed, in_weight, preferred_element_type=jnp.float32).astype(jnp.bfloat16)
    values = projected.astype(jnp.float32).reshape(SEQ, GROUPS, GROUP_DIM)
    totals = jnp.cumsum(values, axis=0)
    padded = jnp.pad(totals, ((16, 0), (0, 0), (0, 0)))
    position = jnp.arange(SEQ, dtype=jnp.int32)[:, None, None]
    group_level = (jnp.arange(GROUPS, dtype=jnp.int32) % 4)[None, :, None]
    window_mean = jnp.zeros((SEQ, GROUPS, GROUP_DIM), jnp.float32)
    for level in range(4):
        width = 2 ** (level + 1)
        sums = totals - padded[16 - width:16 - width + SEQ]
        count = jnp.minimum(position + 1, width).astype(jnp.float32)
        window_mean = jnp.where(group_level == level, sums / count, window_mean)
    pooled = (window_mean - values).astype(jnp.bfloat16)
    mapped = jnp.einsum('sgc,gcd->sgd', pooled.astype(jnp.float32), group_weight.astype(jnp.float32))
    pool_out = (mapped.reshape(SEQ, POOL) * pool_scale).astype(jnp.bfloat16)
    mixed_stream = stream + jnp.dot(pool_out, out_weight, preferred_element_type=jnp.float32)
    normed_two = rms_norm(mixed_stream, norm2_gain).astype(jnp.bfloat16)
    upper = jnp.dot(normed_two, up_weight, preferred_element_type=jnp.float32)
    hidden = jnp.square(jax.nn.relu(upper)).astype(jnp.bfloat16)
    block = FF // N_TP
    channel_sum = jnp.zeros((SEQ, D), jnp.float32)
    for index in range(N_TP):
        partial_sum = jnp.dot(hidden[:, index * block:(index + 1) * block], down_weight[index * block:(index + 1) * block], preferred_element_type=jnp.float32).astype(jnp.bfloat16)
        channel_sum = channel_sum + lax.optimization_barrier(partial_sum).astype(jnp.float32)
    return (mixed_stream + channel_sum).astype(jnp.bfloat16)

def reference(tokens, norm1_gain, in_weight, group_weight, pool_scale, out_weight, norm2_gain, up_weight, down_weight):
    sequences = tokens.reshape(TOKENS // SEQ, SEQ, D)

    def apply(rows):
        return one_sequence(rows, norm1_gain, in_weight, group_weight, pool_scale, out_weight, norm2_gain, up_weight, down_weight)
    return lax.map(apply, sequences).reshape(TOKENS, D)
```

```python
import jax
import jax.numpy as jnp
from jax import lax
from jax.sharding import Mesh
from jax.sharding import PartitionSpec as P

FS = ("zl", "x")
TP = ("y", "c")
Z = ("rep", "zl")
ALL = ("rep", "zl", "x", "y", "c")
HALO = 16
EPS = 1e-06
F32 = jnp.float32
BF16 = jnp.bfloat16


def from_peer(v, axis, n, d):
    return lax.ppermute(v, axis, [((i + d) % n, i) for i in range(n)])


def ring4(v, axis):
    return [v] + [from_peer(v, axis, 4, d) for d in (1, 2, 3)]


def ring_z(v):
    two = [((i + 2) % 8 if i % 2 == 0 else (i - 2) % 8, i) for i in range(8)]
    return [v, from_peer(v, Z, 8, 1), lax.ppermute(v, Z, two), from_peer(v, Z, 8, -1)]


def swap_core(v):
    return lax.ppermute(v, "c", [(0, 1), (1, 0)])


def rms_norm(values, gain):
    scale = lax.rsqrt(jnp.mean(values * values, axis=-1, keepdims=True) + EPS)
    return values * scale * gain


def to_relative(v, zl, x):
    r = v.reshape(v.shape[0], 4, 4, 128)
    return jnp.roll(jnp.roll(r, -zl, 1), -x, 2).reshape(v.shape)


def to_absolute(v, zl, x):
    r = v.reshape(v.shape[0], 4, 4, 128)
    return jnp.roll(jnp.roll(r, zl, 1), x, 2).reshape(v.shape)


def shifted(values, offset):
    return jnp.pad(values, ((offset, 0), (0, 0)))[: values.shape[0]]


def local(tokens, norm1_gain, in_weight, group_weight, pool_scale, out_weight, norm2_gain, up_weight, down_weight):
    zl, x, y, c = (lax.axis_index(a) for a in ("zl", "x", "y", "c"))
    tokens = to_relative(tokens, zl, x)
    gain1 = to_relative(norm1_gain[None], zl, x)
    gain2 = to_relative(norm2_gain[None], zl, x)

    s_hi = lax.reduce_precision(pool_scale, 8, 7)
    s_mid = lax.reduce_precision(pool_scale - s_hi, 8, 7)
    s_lo = pool_scale - s_hi - s_mid
    scale_rows = jnp.stack([s_hi, s_mid, s_lo] + [jnp.zeros_like(s_hi)] * 13).astype(BF16)
    in_x = jnp.concatenate(ring4(in_weight, "x"), 0)
    first = jnp.concatenate([out_weight, group_weight[0], scale_rows], 0)
    first_y = ring4(first, "y")
    in_z = jnp.concatenate(ring_z(in_x), 0)
    out_y = jnp.concatenate([p[:128] for p in first_y], 0)
    out_z = jnp.stack(ring_z(out_y))
    in_y = jnp.concatenate(ring4(in_z, "y"), 1)
    out_x = ring4(out_z, "x")
    out_full = jnp.stack(out_x).transpose(2, 1, 0, 3).reshape(512, 2048)

    other = swap_core(tokens)
    last = jnp.where(c == 1, tokens[-HALO:], other[-HALO:])
    halo = from_peer(last, "y", 4, -1)
    halo = jnp.where(y == 0, jnp.zeros_like(halo), halo)
    lower = jnp.where(c == 0, tokens, other)
    upper = jnp.where(c == 0, other, tokens)
    rows = jnp.concatenate([halo, lower, upper], 0).astype(F32)
    normed = rms_norm(rows, gain1).astype(BF16)
    projected = jnp.dot(normed, in_y, preferred_element_type=F32).astype(BF16)
    values = projected.astype(F32)
    t = (y * 256 + jnp.arange(256, dtype=jnp.int32))[:, None]
    mapped = []
    for dy in range(4):
        level = 2 * ((y + dy) % 2) + c
        v = values[:, dy * 128 : dy * 128 + 128]
        s = v + shifted(v, 1)
        for k in (1, 2, 3):
            s = jnp.where(level >= k, s + shifted(s, 2**k), s)
        count = jnp.minimum(t + 1, jnp.left_shift(2, level)).astype(F32)
        pooled = (s[HALO:] / count - v[HALO:]).astype(BF16)
        piece = first_y[dy]
        scale = piece[256:257].astype(F32) + piece[257:258].astype(F32) + piece[258:259].astype(F32)
        m = jnp.dot(pooled, piece[128:256], preferred_element_type=F32)
        mapped.append((m * scale).astype(BF16))
    pool_out = jnp.concatenate(mapped, 1)
    part = jnp.dot(pool_out, out_full, preferred_element_type=F32)
    mine = jnp.where(c == 0, part[:128], part[128:])
    theirs = jnp.where(c == 0, part[128:], part[:128]).astype(BF16)
    mixed_stream = tokens.astype(F32) + (mine + swap_core(theirs).astype(F32))
    normed_two = rms_norm(mixed_stream, gain2).astype(BF16)

    up_x = jnp.concatenate(ring4(up_weight, "x"), 0)
    down_z = jnp.stack(ring_z(down_weight))
    up_full = jnp.concatenate(ring_z(up_x), 0)
    down_full = jnp.stack(ring4(down_z, "x")).transpose(2, 1, 0, 3).reshape(1024, 2048)

    mine_y = jnp.concatenate(ring4(normed_two, "y"), 0)
    all_rows = jnp.concatenate([mine_y, swap_core(mine_y)], 0)
    hidden = jnp.dot(all_rows, up_full, preferred_element_type=F32)
    hidden = jnp.square(jax.nn.relu(hidden)).astype(BF16)
    partial = jnp.dot(hidden, down_full, preferred_element_type=F32).astype(BF16)
    chip = (partial[:512].astype(F32) + swap_core(partial[512:]).astype(F32)).astype(BF16)
    total = chip[:128].astype(F32)
    for d in (1, 2, 3):
        total = total + from_peer(chip[d * 128 : d * 128 + 128], "y", 4, -d).astype(F32)
    return to_absolute((mixed_stream + total).astype(BF16), zl, x)


def solution(mesh):
    split = Mesh(mesh.devices.reshape(2, 4, 4, 4, 2), ALL)
    in_specs = (
        P(ALL, None),
        P(),
        P(FS, TP),
        P(TP, None, None),
        P(TP),
        P(TP, FS),
        P(),
        P(FS, TP),
        P(TP, FS),
    )
    return jax.shard_map(local, mesh=split, in_specs=in_specs, out_specs=P(ALL, None), check_vma=False)
```
